32 devices in a mesh: kv: 8 (over z, x), tp: 4 (over y, core).
Axes of the slice: x: 2, y: 2, z: 4, core: 2. Of those that a mesh axis runs over, the one named last changes fastest.
Arguments:
- tokens: bfloat16 [4096, 2048], P(('kv', 'tp')), may hold values from -6 to 6
- query_weight: bfloat16 [2048, 1024], P(None, 'tp'), may hold values from -0.125 to 0.125
- latent_weight: bfloat16 [2048, 256], replicated, may hold values from -0.125 to 0.125
- key_absorb: bfloat16 [8, 128, 256], P('tp'), may hold values from -0.5 to 0.5
- query_gain: bfloat16 [256], replicated, may hold values from 0.4 to 8
- latent_gain: bfloat16 [256], replicated, may hold values from 0.4 to 8
- value_absorb: bfloat16 [8, 256, 128], P('tp'), may hold values from -0.375 to 0.375
- head_gain: bfloat16 [8, 128], P('tp'), may hold values from 0.099609375 to 1.8984375
- out_weight: bfloat16 [1024, 2048], P('tp'), may hold values from -0.1875 to 0.1875
- chosen: int32 [64, 11], P('kv'), may hold values from 0 to 63, as said below
Outputs:
- mixed_out: bfloat16 [4096, 2048], P(('kv', 'tp'))
The draws below stay inside these ranges and needn't reach their ends.
Inputs may be any that keep to these rules, and one draw needn't show every extreme that they name: `chosen`: entry 0 of row b is b; a row's entries are distinct. Entries 1 to 3 lie in the same aligned run of 8 block numbers as b, the other 7 in other runs. For each aligned run of 8 rows and each other aligned run of 8 block numbers, those rows together name at most one block of that run. Entries above the row's own number may occur and contribute nothing.
All inputs are finite; a program needn't handle non-finite values.
Results may differ from the reference program's by a relative error of at most 0.014.
The reference program's roundings to bfloat16 on the way count: a program that leaves them out, or rounds other values in their place, can miss the bound.
Values may be sent and summed in bfloat16 or wider, within the bound.
A program may use at most 64 MiB of HBM per device.

```python
import jax
import jax.numpy as jnp
from jax import lax

D = 2048
HEADS = 8
HEAD = 128
LATENT = 256
BLOCK = 64
TOKENS = 4096
NBLK = 64
SPAN_BLOCKS = 8
LOCAL_PICKS = 3
REMOTE = 7
NSEL = 11
HEAD_GROUP = 2
N_TP = 4


def gain_values(key, salt):
    base = jax.random.fold_in(key, salt)
    return jnp.clip(1.0 + 0.18 * jax.random.normal(base, (LATENT,), jnp.float32), 0.4, 1.6).astype(jnp.bfloat16)


def draw_query_gain(key, part):
    return gain_values(key, 11)


def draw_latent_gain(key, part):
    return gain_values(key, 23)


def draw_chosen(key, part):
    owners = NBLK // SPAN_BLOCKS
    first_key = jax.random.fold_in(key, 101)
    second_key = jax.random.fold_in(key, 202)
    third_key = jax.random.fold_in(key, 303)
    fourth_key = jax.random.fold_in(key, 404)
    block_pick = jax.random.randint(first_key, (owners, owners), 0, SPAN_BLOCKS)
    favored = (jax.random.randint(second_key, (owners,), 0, 4) == 0).astype(jnp.int32)
    row_ids = jnp.arange(NBLK, dtype=jnp.int32)
    device_of = row_ids // SPAN_BLOCKS
    local_pos = row_ids % SPAN_BLOCKS
    local_noise = jax.random.randint(third_key, (NBLK, SPAN_BLOCKS), 0, 1 << 20)
    local_range = jnp.arange(SPAN_BLOCKS, dtype=jnp.int32)
    local_score = local_noise * SPAN_BLOCKS + local_range[None, :]
    local_score = jnp.where(local_range[None, :] == local_pos[:, None], -1, local_score)
    _, local_pick = lax.top_k(local_score, LOCAL_PICKS)
    local_ids = device_of[:, None] * SPAN_BLOCKS + local_pick.astype(jnp.int32)
    owner_range = jnp.arange(owners, dtype=jnp.int32)
    remote_noise = jax.random.randint(fourth_key, (NBLK, owners), 0, 1 << 12)
    earlier = owner_range[None, :] < device_of[:, None]
    forced = (owner_range[None, :] == device_of[:, None] - 1) | (owner_range[None, :] == device_of[:, None] - owners // 2)
    level = jnp.where(forced, 3, jnp.where(earlier, 1, 0))
    level = jnp.where(owner_range[None, :] == device_of[:, None], -1, level)
    remote_score = (level * (1 << 13) + remote_noise + favored[None, :] * (1 << 11)) * owners + owner_range[None, :]
    _, remote_pick = lax.top_k(remote_score, REMOTE)
    remote_pick = remote_pick.astype(jnp.int32)
    remote_ids = remote_pick * SPAN_BLOCKS + block_pick[device_of[:, None], remote_pick]
    return jnp.concatenate([row_ids[:, None], local_ids, remote_ids], axis=1).astype(jnp.int32)


def block_scale(rng, dims, split, least, top_value):
    factor_of = 1.0
    for position, blocks in split:
        heights = jax.random.uniform(jax.random.fold_in(jax.random.fold_in(rng, 6), position), (blocks,), jnp.float32, least / len(split), top_value / len(split))
        factor_of = factor_of * jnp.repeat(jnp.exp(heights), dims[position] // blocks).reshape((-1,) + (1,) * (len(dims) - 1 - position))
    return factor_of


def scatter_about(stream_key, dims, width, reach, split=(), kind=jnp.bfloat16):
    values = jax.random.normal(stream_key, dims, jnp.float32) * width
    if len(split) > 0:
        values = block_scale(stream_key, dims, split, -0.22, 0.18) * values
    return jnp.clip(values, min=-reach, max=reach).astype(kind)


def setup_inputs(seed: int = 0) -> dict:
    keys = jax.random.split(jax.random.key(seed), 11)
    tokens = scatter_about(keys[0], (TOKENS, D), 1.0, 6.0, ((0, 32),))
    query_weight = scatter_about(keys[1], (D, HEADS * HEAD), D ** -0.5, 0.125, ((1, 4),))
    latent_weight = scatter_about(keys[2], (D, LATENT), D ** -0.5, 0.125)
    key_absorb = scatter_about(keys[3], (HEADS, HEAD, LATENT), HEAD ** -0.5, 0.5, ((0, 4),))
    query_gain = draw_query_gain(jax.random.fold_in(keys[10], 71), 0)
    latent_gain = draw_latent_gain(jax.random.fold_in(keys[10], 71), 0)
    value_absorb = scatter_about(keys[6], (HEADS, LATENT, HEAD), LATENT ** -0.5, 0.375, ((0, 4),))
    head_gain = jnp.clip(1.0 + 0.18 * jax.random.normal(keys[7], (HEADS, HEAD), jnp.float32), 0.099609375, 1.8984375).astype(jnp.bfloat16)
    out_weight = scatter_about(keys[8], (HEADS * HEAD, D), (HEADS * HEAD) ** -0.5, 0.1875, ((0, 4),))
    chosen = draw_chosen(jax.random.fold_in(keys[10], 71), 0)
    return {"tokens": tokens, "query_weight": query_weight, "latent_weight": latent_weight, "key_absorb": key_absorb, "query_gain": query_gain, "latent_gain": latent_gain, "value_absorb": value_absorb, "head_gain": head_gain, "out_weight": out_weight, "chosen": chosen}


epsilon = 1e-06

def normalize(values, gain):
    return values * lax.rsqrt(lax.optimization_barrier(jnp.mean(values * values, axis=-1, keepdims=True)) + epsilon) * gain

def reference(tokens, query_weight, latent_weight, key_absorb, query_gain, latent_gain, value_absorb, head_gain, out_weight, chosen):
    queries = jnp.dot(tokens, query_weight, preferred_element_type=jnp.float32).astype(jnp.bfloat16)
    latent = normalize(jnp.dot(tokens, latent_weight, preferred_element_type=jnp.float32), latent_gain.astype(jnp.float32)).astype(jnp.bfloat16)
    head_query = queries.reshape(TOKENS, HEADS, HEAD).astype(jnp.float32)
    absorbed = jnp.einsum('thd,hdc->thc', head_query, key_absorb.astype(jnp.float32))
    absorbed = normalize(absorbed, query_gain.astype(jnp.float32)).astype(jnp.bfloat16)
    key_blocks = latent.reshape(NBLK, BLOCK, LATENT)
    query_blocks = absorbed.reshape(NBLK, BLOCK, HEADS, LATENT)
    offsets = jnp.arange(BLOCK, dtype=jnp.int32)

    def attend(inputs):
        row_block, picked, block_index = inputs
        key_rows = key_blocks[picked].reshape(NSEL * BLOCK, LATENT).astype(jnp.float32)
        scores = jnp.einsum('qhc,kc->hqk', row_block.astype(jnp.float32), key_rows) * LATENT ** (-0.5)
        key_pos = (picked[:, None] * BLOCK + offsets[None, :]).reshape(NSEL * BLOCK)
        query_pos = block_index * BLOCK + offsets
        visible = key_pos[None, :] <= query_pos[:, None]
        scores = jnp.where(visible[None], scores, -jnp.inf)
        weights = lax.optimization_barrier(jax.nn.softmax(scores, axis=-1).astype(jnp.bfloat16)).astype(jnp.float32)
        return jnp.einsum('hqk,kc->qhc', weights, key_rows).astype(jnp.bfloat16)
    mixed = lax.map(attend, (query_blocks, chosen, jnp.arange(NBLK, dtype=jnp.int32)))
    mixed = mixed.reshape(TOKENS, HEADS, LATENT).astype(jnp.float32)
    values = jnp.einsum('thc,hcd->thd', mixed, value_absorb.astype(jnp.float32))
    head_out = normalize(values, head_gain.astype(jnp.float32)).astype(jnp.bfloat16).reshape(TOKENS, HEADS * HEAD)
    group_width = HEAD_GROUP * HEAD
    accumulated = jnp.zeros((TOKENS, D), jnp.float32)
    for group_index in range(N_TP):
        low = group_index * group_width
        partial_value = jnp.dot(head_out[:, low:low + group_width], out_weight[low:low + group_width], preferred_element_type=jnp.float32)
        accumulated = accumulated + lax.optimization_barrier(partial_value.astype(jnp.bfloat16)).astype(jnp.float32)
    return accumulated.astype(jnp.bfloat16)
```

```python
import functools
import math

import jax
import jax.numpy as jnp
from jax import lax
from jax.experimental import pallas as pl
from jax.experimental.pallas import tpu as pltpu
from jax.sharding import PartitionSpec as P

epsilon = 1e-06
LOCAL = 4
SPLIT = 2
MESH = pl.DeviceIdType.MESH


def normalize(values, gain):
    return values * lax.rsqrt(jnp.mean(values * values, axis=-1, keepdims=True) + epsilon) * gain


def kernel(
    n_kv,
    tok_hbm,
    qw_hbm,
    lw_hbm,
    ka_hbm,
    qg_hbm,
    lg_hbm,
    va_hbm,
    hg_hbm,
    ow_hbm,
    ch_hbm,
    out,
    tok,
    qw,
    lw,
    ka,
    va,
    ow,
    qg_ref,
    lg_ref,
    hg_ref,
    ch_s,
    ch_v,
    lat,
    rem,
    stage,
    req,
    qabs,
    pre_out,
    pre_in,
    y_out,
    y_in,
    p_out,
    p_in,
    ld,
    tok_s,
    tok_r,
    lat_s,
    lat_r,
    req_s,
    req_r,
    blk_s,
    blk_r,
    share_s,
    share_r,
    red_s,
    red_r,
):
    kv = lax.axis_index("kv")
    t = lax.axis_index("tp")
    pair, core = t // 2, t % 2
    t1 = pair * 2 + (1 - core)
    t2 = (1 - pair) * 2 + core
    t3 = (1 - pair) * 2 + (1 - core)
    nblk, block, latent = lat.shape
    heads, head = ka.shape[0], ka.shape[1]
    rows = tok.shape[1]
    bpd = rows // block
    half = block // 2
    picks = ch_s.shape[1]
    f32, bf16 = jnp.float32, jnp.bfloat16

    loads = [
        pltpu.make_async_copy(src, dst, ld.at[i])
        for i, (src, dst) in enumerate(
            (
                (tok_hbm, tok.at[t]),
                (ch_hbm, ch_v),
                (lw_hbm, lw),
                (lg_hbm, lg_ref),
                (qw_hbm, qw),
                (ka_hbm, ka),
                (qg_hbm, qg_ref),
                (ch_hbm, ch_s),
                (va_hbm, va),
                (hg_hbm, hg_ref),
                (ow_hbm, ow),
            )
        )
    ]
    for load in loads:
        load.start()

    barrier = pltpu.get_barrier_semaphore()
    for peer in (t1, t2, t3):
        pl.semaphore_signal(barrier, inc=1, device_id={"tp": peer}, device_id_type=MESH)

    def greet(i, carry):
        @pl.when(kv + i < n_kv)
        def _():
            pl.semaphore_signal(
                barrier, inc=1, device_id={"kv": kv + i}, device_id_type=MESH
            )

        return carry

    lax.fori_loop(1, n_kv, greet, 0)
    loads[0].wait()
    loads[2].wait()
    loads[3].wait()
    own_latent = normalize(
        jnp.dot(tok[t], lw[...], preferred_element_type=f32),
        lg_ref[...].astype(f32).reshape(1, latent),
    ).astype(bf16)
    lat[pl.ds(t * bpd, bpd)] = own_latent.reshape(bpd, block, latent)
    loads[1].wait()
    pl.semaphore_wait(barrier, kv + 3)

    def send(src, dst, ss, rs, where):
        return pltpu.make_async_remote_copy(
            src_ref=src, dst_ref=dst, send_sem=ss, recv_sem=rs, device_id=where, device_id_type=MESH
        )

    def tok_part(r, c):
        return tok.at[r, pl.ds(c * block, block)]

    def tok_copy(kind, r, c, peer):
        return send(
            tok_part(r, c), tok_part(r, c), tok_s.at[kind, c], tok_r.at[kind, c], {"tp": peer}
        )

    far = [tok_copy(1, t, c, t2) for c in range(bpd)]
    near = [tok_copy(0, t, c, t1) for c in range(bpd)]
    relay = [tok_copy(2, t2, c, t1) for c in range(bpd)]
    own_lat = lat.at[pl.ds(t * bpd, bpd)]
    cross_lat = lat.at[pl.ds(t2 * bpd, bpd)]
    lat_copies = [
        send(own_lat, own_lat, lat_s.at[0], lat_r.at[0], {"tp": t2}),
        send(own_lat, own_lat, lat_s.at[1], lat_r.at[1], {"tp": t1}),
        send(cross_lat, cross_lat, lat_s.at[2], lat_r.at[2], {"tp": t1}),
    ]
    lat_copies[0].start()
    lat_copies[1].start()

    def req_copy(i, owner, peer):
        return send(ch_v, req.at[owner], req_s.at[i], req_r.at[i], {"kv": peer})

    def ask(i, carry):
        @pl.when(kv >= i)
        def _():
            req_copy(i, kv, kv - i).start()

        return carry

    lax.fori_loop(1, n_kv, ask, 0)

    for copy in far + near:
        copy.start()

    for load in loads[4:7]:
        load.wait()
    query_gain = qg_ref[...].astype(f32).reshape(1, latent)

    def project(r, start, count):
        queries = jnp.dot(
            tok[r, pl.ds(start, count), :], qw[...], preferred_element_type=f32
        ).astype(bf16)
        for h in range(heads):
            absorbed = jnp.dot(
                queries[:, h * head : (h + 1) * head], ka[h], preferred_element_type=f32
            )
            qabs[h, pl.ds(r * rows + start, count), :] = normalize(absorbed, query_gain).astype(bf16)

    lat_copies[0].wait_recv()
    lat_copies[2].start()
    lat_copies[1].wait_recv()
    lat_copies[2].wait_recv()

    def blk_copy(i, owner, peer):
        return send(stage.at[peer], rem.at[owner, core], blk_s.at[i], blk_r.at[i], {"kv": peer})

    def share_copy(i, owner):
        part = rem.at[owner, core]
        return send(part, part, share_s.at[i], share_r.at[i], {"tp": t1})

    def serve(i, carry):
        peer = kv + i

        @pl.when(peer < n_kv)
        def _():
            req_copy(i, peer, peer).wait_recv()
            wanted = req[peer]
            local = jnp.max(jnp.where(lax.div(wanted, nblk) == kv, lax.rem(wanted, nblk), 0))
            stage[peer] = jnp.where(core == 0, lat[local, :half], lat[local, half:])
            blk_copy(i, kv, peer).start()

        return carry

    rem[kv] = jnp.zeros((2, half, latent), bf16)

    project(t, 0, rows)
    for copy in near:
        copy.wait_recv()
    project(t1, 0, rows)
    lax.fori_loop(1, n_kv, serve, 0)

    def fetch(c):
        tok_copy(1, t2, c, t2).wait_recv()
        relay[c].start()
        project(t2, c * block, block)
        tok_copy(2, t3, c, t1).wait_recv()
        project(t3, c * block, block)

    fetch(0)

    def arrive(i, carry):
        @pl.when(kv >= i)
        def _():
            blk_copy(i, kv - i, kv - i).wait_recv()
            share_copy(i, kv - i).start()

        return carry

    lax.fori_loop(1, n_kv, arrive, 0)

    def arrive_shared(i, carry):
        @pl.when(kv >= i)
        def _():
            share_copy(i, kv - i).wait_recv()

        return carry

    lax.fori_loop(1, n_kv, arrive_shared, 0)
    for load in loads[7:]:
        load.wait()

    length = picks * block
    column = lax.broadcasted_iota(jnp.int32, (1, length), 1) // block
    lead = min(128, length)
    row_in = lax.rem(lax.broadcasted_iota(jnp.int32, (heads * block, lead), 0), block)
    col_in = lax.broadcasted_iota(jnp.int32, (heads * block, lead), 1)
    causal = jnp.where((col_in < block) & (col_in > row_in), -jnp.inf, 0.0).astype(f32)
    factor = latent ** (-0.5) * math.log2(math.e)
    head_gain = hg_ref[...].astype(f32)

    def attend(r, c):
        j = r * bpd + c
        b = kv * nblk + j
        q = qabs[:, pl.ds(j * block, block), :].reshape(heads * block, latent)
        parts = [lat[j]]
        bias = jnp.zeros((1, length), f32)
        for p in range(1, picks):
            pick = ch_s[j, p]
            seen = pick < b
            if p < LOCAL:
                parts.append(lat[jnp.where(seen, lax.rem(pick, nblk), j)])
            else:
                parts.append(rem[jnp.where(seen, lax.div(pick, nblk), kv)].reshape(block, latent))
            bias = jnp.where(column == p, jnp.where(seen, 0.0, -jnp.inf).astype(f32), bias)
        keys = jnp.concatenate(parts, axis=0)
        scores = (
            lax.dot_general(q, keys, (((1,), (1,)), ((), ())), preferred_element_type=f32) * factor
            + bias
        )
        scores = jnp.concatenate([scores[:, :lead] + causal, scores[:, lead:]], axis=1)
        top = jnp.max(scores, axis=-1, keepdims=True)
        weights = jnp.exp2(scores - top)
        total = jnp.sum(weights, axis=-1, keepdims=True)
        mixed = jnp.dot(weights.astype(bf16), keys, preferred_element_type=f32)
        mixed = (mixed / total).astype(bf16)
        outs = []
        for h in range(heads):
            values = jnp.dot(
                mixed[h * block : (h + 1) * block], va[h], preferred_element_type=f32
            )
            outs.append(normalize(values, head_gain[h : h + 1]).astype(bf16))
        return jnp.concatenate(outs, axis=1)

    def red_copy(kind, c, k, src, dst, peer):
        return send(
            src.at[c, k], dst.at[c, k], red_s.at[kind, c, k], red_r.at[kind, c, k], {"tp": peer}
        )

    piece = out.shape[1] // SPLIT
    cols = [slice(k * piece, (k + 1) * piece) for k in range(SPLIT)]
    reds = []

    def project_out(gathered, k):
        return jnp.dot(gathered, ow[:, cols[k]], preferred_element_type=f32).astype(bf16)

    def emit(kind, c, k, src, dst, peer, value):
        src[c, k] = value
        copy = red_copy(kind, c, k, src, dst, peer)
        copy.start()
        reds.append(copy)
        return copy

    for c in range(bpd):
        if c > 0:
            fetch(c)
        heads_out = attend(t3, c)
        pre = [emit(0, c, k, pre_out, pre_in, t1, project_out(heads_out, k)) for k in range(SPLIT)]
        heads_out = attend(t2, c)
        for k in range(SPLIT):
            mine = project_out(heads_out, k).astype(f32)
            pre[k].wait_recv()
            emit(1, c, k, y_out, y_in, t2, (mine + pre_in[c, k].astype(f32)).astype(bf16))
    for c in range(bpd):
        heads_out = attend(t1, c)
        for k in range(SPLIT):
            emit(2, c, k, p_out, p_in, t1, project_out(heads_out, k))
    for c in range(bpd):
        heads_out = attend(t, c)
        for k in range(SPLIT):
            out[pl.ds(c * block, block), cols[k]] = project_out(heads_out, k)
    for c in range(bpd):
        for k in range(SPLIT):
            red_copy(2, c, k, p_out, p_in, t1).wait_recv()
            red_copy(1, c, k, y_out, y_in, t2).wait_recv()
            place = pl.ds(c * block, block)
            out[place, cols[k]] = (
                out[place, cols[k]].astype(f32) + p_in[c, k].astype(f32) + y_in[c, k].astype(f32)
            ).astype(bf16)

    for copy in far + near + relay + lat_copies + reds:
        copy.wait_send()

    def finish(i, carry):
        @pl.when(kv >= i)
        def _():
            req_copy(i, kv, kv - i).wait_send()
            share_copy(i, kv - i).wait_send()

        @pl.when(kv + i < n_kv)
        def _():
            blk_copy(i, kv, kv + i).wait_send()

        return carry

    lax.fori_loop(1, n_kv, finish, 0)


def body(n_kv, n_tp, tokens, qw, lw, ka, qg, lg, va, hg, ow, chosen):
    rows, width = tokens.shape
    nblk = chosen.shape[0]
    block = rows * n_tp // nblk
    latent = lw.shape[1]
    bpd = rows // block
    bf16 = jnp.bfloat16
    hbm = pl.BlockSpec(memory_space=pltpu.HBM)
    vmem = pl.BlockSpec(memory_space=pltpu.VMEM)
    dma = pltpu.SemaphoreType.DMA
    piece = pltpu.VMEM((bpd, SPLIT, block, ow.shape[1] // SPLIT), bf16)
    arrays = [pltpu.with_memory_space_constraint(a, pltpu.HBM) for a in (tokens, qw, lw, ka, qg, lg, va, hg, ow, chosen)]
    return pl.pallas_call(
        functools.partial(kernel, n_kv),
        out_shape=jax.ShapeDtypeStruct((rows, ow.shape[1]), bf16),
        in_specs=[hbm] * 10,
        out_specs=vmem,
        scratch_shapes=[
            pltpu.VMEM((n_tp, rows, width), bf16),
            pltpu.VMEM(qw.shape, bf16),
            pltpu.VMEM(lw.shape, bf16),
            pltpu.VMEM(ka.shape, bf16),
            pltpu.VMEM(va.shape, bf16),
            pltpu.VMEM(ow.shape, bf16),
            pltpu.VMEM(qg.shape, bf16),
            pltpu.VMEM(lg.shape, bf16),
            pltpu.VMEM(hg.shape, bf16),
            pltpu.SMEM(chosen.shape, jnp.int32),
            pltpu.VMEM(chosen.shape, jnp.int32),
            pltpu.VMEM((nblk, block, latent), bf16),
            pltpu.VMEM((n_kv, 2, block // 2, latent), bf16),
            pltpu.VMEM((n_kv, block // 2, latent), bf16),
            pltpu.VMEM((n_kv,) + chosen.shape, jnp.int32),
            pltpu.VMEM((ka.shape[0], rows * n_tp, latent), bf16),
            piece,
            piece,
            piece,
            piece,
            piece,
            piece,
            dma((11,)),
            dma((3, bpd)),
            dma((3, bpd)),
            dma((3,)),
            dma((3,)),
            dma((n_kv,)),
            dma((n_kv,)),
            dma((n_kv,)),
            dma((n_kv,)),
            dma((n_kv,)),
            dma((n_kv,)),
            dma((3, bpd, SPLIT)),
            dma((3, bpd, SPLIT)),
        ],
        compiler_params=pltpu.CompilerParams(
            collective_id=0, has_side_effects=True, vmem_limit_bytes=50000000
        ),
    )(*arrays)


def solution(mesh):
    return jax.shard_map(
        functools.partial(body, mesh.shape["kv"], mesh.shape["tp"]),
        mesh=mesh,
        in_specs=(
            P(("kv", "tp"), None),
            P(None, "tp"),
            P(),
            P("tp", None, None),
            P(),
            P(),
            P("tp", None, None),
            P("tp", None),
            P("tp", None),
            P("kv", None),
        ),
        out_specs=P(("kv", "tp"), None),
        check_vma=False,
    )
```

```python
import functools
import math

import jax
import jax.numpy as jnp
from jax import lax
from jax.experimental import pallas as pl
from jax.experimental.pallas import tpu as pltpu
from jax.sharding import PartitionSpec as P

epsilon = 1e-06
LOCAL = 4
SPLIT = 2
EARLY = 16
MESH = pl.DeviceIdType.MESH


def normalize(values, gain):
    return values * lax.rsqrt(jnp.mean(values * values, axis=-1, keepdims=True) + epsilon) * gain


def kernel(
    n_kv,
    tok_hbm,
    qw_hbm,
    lw_hbm,
    ka_hbm,
    qg_hbm,
    lg_hbm,
    va_hbm,
    hg_hbm,
    ow_hbm,
    ch_hbm,
    out,
    tok,
    qw,
    lw,
    ka,
    va,
    ow,
    qg_ref,
    lg_ref,
    hg_ref,
    ch_s,
    ch_v,
    lat,
    rem,
    stage,
    req,
    qabs,
    pre_out,
    pre_in,
    y_out,
    y_in,
    p_out,
    p_in,
    ld,
    tok_s,
    tok_r,
    early_s,
    early_r,
    lat_s,
    lat_r,
    req_s,
    req_r,
    blk_s,
    blk_r,
    share_s,
    share_r,
    red_s,
    red_r,
):
    kv = lax.axis_index("kv")
    t = lax.axis_index("tp")
    pair, core = t // 2, t % 2
    t1 = pair * 2 + (1 - core)
    t2 = (1 - pair) * 2 + core
    t3 = (1 - pair) * 2 + (1 - core)
    nblk, block, latent = lat.shape
    heads, head = ka.shape[0], ka.shape[1]
    rows = tok.shape[1]
    bpd = rows // block
    half = block // 2
    picks = ch_s.shape[1]
    f32, bf16 = jnp.float32, jnp.bfloat16

    loads = [
        pltpu.make_async_copy(src, dst, ld.at[i])
        for i, (src, dst) in enumerate(
            (
                (tok_hbm, tok.at[t]),
                (ch_hbm, ch_v),
                (lw_hbm, lw),
                (lg_hbm, lg_ref),
                (qw_hbm, qw),
                (ka_hbm, ka),
                (qg_hbm, qg_ref),
                (ch_hbm, ch_s),
                (va_hbm, va),
                (hg_hbm, hg_ref),
                (ow_hbm, ow),
            )
        )
    ]
    for load in loads:
        load.start()

    barrier = pltpu.get_barrier_semaphore()
    for peer in (t1, t2, t3):
        pl.semaphore_signal(barrier, inc=1, device_id={"tp": peer}, device_id_type=MESH)

    def greet(i, carry):
        @pl.when(kv + i < n_kv)
        def _():
            pl.semaphore_signal(
                barrier, inc=1, device_id={"kv": kv + i}, device_id_type=MESH
            )

        return carry

    lax.fori_loop(1, n_kv, greet, 0)
    def send(src, dst, ss, rs, where):
        return pltpu.make_async_remote_copy(
            src_ref=src, dst_ref=dst, send_sem=ss, recv_sem=rs, device_id=where, device_id_type=MESH
        )

    def early_copy(r):
        part = tok.at[r, pl.ds(0, EARLY)]
        return send(part, part, early_s.at[0], early_r.at[0], {"tp": t2})

    loads[0].wait()
    loads[2].wait()
    loads[3].wait()
    own_latent = normalize(
        jnp.dot(tok[t], lw[...], preferred_element_type=f32),
        lg_ref[...].astype(f32).reshape(1, latent),
    ).astype(bf16)
    lat[pl.ds(t * bpd, bpd)] = own_latent.reshape(bpd, block, latent)
    pl.semaphore_wait(barrier, kv + 3)
    loads[1].wait()

    def req_copy(i, owner, peer):
        return send(ch_v, req.at[owner], req_s.at[i], req_r.at[i], {"kv": peer})

    def ask(i, carry):
        @pl.when(kv >= i)
        def _():
            req_copy(i, kv, kv - i).start()

        return carry

    lax.fori_loop(1, n_kv, ask, 0)

    def tok_part(r, c, kind):
        start = EARLY if kind == 1 and c == 0 else c * block
        return tok.at[r, pl.ds(start, (c + 1) * block - start)]

    def tok_copy(kind, r, c, peer):
        return send(
            tok_part(r, c, kind), tok_part(r, c, kind), tok_s.at[kind, c], tok_r.at[kind, c], {"tp": peer}
        )

    far = [tok_copy(1, t, c, t2) for c in range(bpd)]
    near = [tok_copy(0, t, c, t1) for c in range(bpd)]
    relay = [tok_copy(2, t2, c, t1) for c in range(bpd)]
    own_lat = lat.at[pl.ds(t * bpd, bpd)]
    cross_lat = lat.at[pl.ds(t2 * bpd, bpd)]
    lat_copies = [
        send(own_lat, own_lat, lat_s.at[0], lat_r.at[0], {"tp": t2}),
        send(own_lat, own_lat, lat_s.at[1], lat_r.at[1], {"tp": t1}),
        send(cross_lat, cross_lat, lat_s.at[2], lat_r.at[2], {"tp": t1}),
    ]
    lat_copies[0].start()
    lat_copies[1].start()
    early_copy(t).start()

    for copy in far + near:
        copy.start()

    for load in loads[4:7]:
        load.wait()
    query_gain = qg_ref[...].astype(f32).reshape(1, latent)

    def project(r, start, count):
        queries = jnp.dot(
            tok[r, pl.ds(start, count), :], qw[...], preferred_element_type=f32
        ).astype(bf16)
        for h in range(heads):
            absorbed = jnp.dot(
                queries[:, h * head : (h + 1) * head], ka[h], preferred_element_type=f32
            )
            qabs[h, pl.ds(r * rows + start, count), :] = normalize(absorbed, query_gain).astype(bf16)

    lat_copies[0].wait_recv()
    lat_copies[2].start()
    lat_copies[1].wait_recv()
    lat_copies[2].wait_recv()

    def blk_copy(i, owner, peer):
        return send(stage.at[peer], rem.at[owner, core], blk_s.at[i], blk_r.at[i], {"kv": peer})

    def share_copy(i, owner):
        part = rem.at[owner, core]
        return send(part, part, share_s.at[i], share_r.at[i], {"tp": t1})

    def serve(i, carry):
        peer = kv + i

        @pl.when(peer < n_kv)
        def _():
            req_copy(i, peer, peer).wait_recv()
            wanted = req[peer]
            local = jnp.max(jnp.where(lax.div(wanted, nblk) == kv, lax.rem(wanted, nblk), 0))
            stage[peer] = jnp.where(core == 0, lat[local, :half], lat[local, half:])
            blk_copy(i, kv, peer).start()

        return carry

    rem[kv] = jnp.zeros((2, half, latent), bf16)

    project(t, 0, rows)
    for copy in near:
        copy.wait_recv()
    project(t1, 0, rows)
    lax.fori_loop(1, n_kv, serve, 0)

    def fetch_cross(c):
        if c == 0:
            early_copy(t2).wait_recv()
        tok_copy(1, t2, c, t2).wait_recv()
        relay[c].start()

    def fetch_relayed(c):
        tok_copy(2, t3, c, t1).wait_recv()
        project(t3, c * block, block)

    def arrive(i, carry):
        @pl.when(kv >= i)
        def _():
            blk_copy(i, kv - i, kv - i).wait_recv()
            share_copy(i, kv - i).start()

        return carry

    late = kv // ((n_kv + 1) // 2)
    ready = 1 + (n_kv - 1) * (1 - late)
    lax.fori_loop(1, ready, arrive, 0)
    fetch_cross(0)
    lax.fori_loop(ready, n_kv, arrive, 0)
    project(t2, 0, block)

    def arrive_shared(i, carry):
        @pl.when(kv >= i)
        def _():
            share_copy(i, kv - i).wait_recv()

        return carry

    lax.fori_loop(1, n_kv, arrive_shared, 0)
    for load in loads[7:]:
        load.wait()

    length = picks * block
    column = lax.broadcasted_iota(jnp.int32, (1, length), 1) // block
    lead = min(128, length)
    row_in = lax.rem(lax.broadcasted_iota(jnp.int32, (heads * block, lead), 0), block)
    col_in = lax.broadcasted_iota(jnp.int32, (heads * block, lead), 1)
    causal = jnp.where((col_in < block) & (col_in > row_in), -jnp.inf, 0.0).astype(f32)
    factor = latent ** (-0.5) * math.log2(math.e)
    head_gain = hg_ref[...].astype(f32)

    def attend(r, c):
        j = r * bpd + c
        b = kv * nblk + j
        q = qabs[:, pl.ds(j * block, block), :].reshape(heads * block, latent)
        parts = [lat[j]]
        bias = jnp.zeros((1, length), f32)
        for p in range(1, picks):
            pick = ch_s[j, p]
            seen = pick < b
            if p < LOCAL:
                parts.append(lat[jnp.where(seen, lax.rem(pick, nblk), j)])
            else:
                parts.append(rem[jnp.where(seen, lax.div(pick, nblk), kv)].reshape(block, latent))
            bias = jnp.where(column == p, jnp.where(seen, 0.0, -jnp.inf).astype(f32), bias)
        keys = jnp.concatenate(parts, axis=0)
        scores = (
            lax.dot_general(q, keys, (((1,), (1,)), ((), ())), preferred_element_type=f32) * factor
            + bias
        )
        scores = jnp.concatenate([scores[:, :lead] + causal, scores[:, lead:]], axis=1)
        top = jnp.max(scores, axis=-1, keepdims=True)
        weights = jnp.exp2(scores - top)
        total = jnp.sum(weights, axis=-1, keepdims=True)
        mixed = jnp.dot(weights.astype(bf16), keys, preferred_element_type=f32)
        mixed = (mixed / total).astype(bf16)
        outs = []
        for h in range(heads):
            values = jnp.dot(
                mixed[h * block : (h + 1) * block], va[h], preferred_element_type=f32
            )
            outs.append(normalize(values, head_gain[h : h + 1]).astype(bf16))
        return jnp.concatenate(outs, axis=1)

    def red_copy(kind, c, k, src, dst, peer):
        return send(
            src.at[c, k], dst.at[c, k], red_s.at[kind, c, k], red_r.at[kind, c, k], {"tp": peer}
        )

    piece = out.shape[1] // SPLIT
    cols = [slice(k * piece, (k + 1) * piece) for k in range(SPLIT)]
    reds = []

    def project_out(gathered, k):
        return jnp.dot(gathered, ow[:, cols[k]], preferred_element_type=f32).astype(bf16)

    def emit(kind, c, k, src, dst, peer, value):
        src[c, k] = value
        copy = red_copy(kind, c, k, src, dst, peer)
        copy.start()
        reds.append(copy)
        return copy

    for c in range(bpd):
        if c > 0:
            fetch_cross(c)
            project(t2, c * block, block)
        heads_out = attend(t2, c)
        pre = [emit(0, c, k, pre_out, pre_in, t1, project_out(heads_out, k)) for k in range(SPLIT)]
        fetch_relayed(c)
        heads_out = attend(t3, c)
        for k in range(SPLIT):
            theirs = project_out(heads_out, k).astype(f32)
            pre[k].wait_recv()
            emit(1, c, k, y_out, y_in, t3, (theirs + pre_in[c, k].astype(f32)).astype(bf16))
    for c in range(bpd):
        heads_out = attend(t1, c)
        for k in range(SPLIT):
            emit(2, c, k, p_out, p_in, t1, project_out(heads_out, k))
    for c in range(bpd):
        heads_out = attend(t, c)
        for k in range(SPLIT):
            out[pl.ds(c * block, block), cols[k]] = project_out(heads_out, k)
    for c in range(bpd):
        for k in range(SPLIT):
            red_copy(2, c, k, p_out, p_in, t1).wait_recv()
            red_copy(1, c, k, y_out, y_in, t3).wait_recv()
            place = pl.ds(c * block, block)
            out[place, cols[k]] = (
                out[place, cols[k]].astype(f32) + p_in[c, k].astype(f32) + y_in[c, k].astype(f32)
            ).astype(bf16)

    early_copy(t).wait_send()
    for copy in far + near + relay + lat_copies + reds:
        copy.wait_send()

    def finish(i, carry):
        @pl.when(kv >= i)
        def _():
            req_copy(i, kv, kv - i).wait_send()
            share_copy(i, kv - i).wait_send()

        @pl.when(kv + i < n_kv)
        def _():
            blk_copy(i, kv, kv + i).wait_send()

        return carry

    lax.fori_loop(1, n_kv, finish, 0)


def body(n_kv, n_tp, tokens, qw, lw, ka, qg, lg, va, hg, ow, chosen):
    rows, width = tokens.shape
    nblk = chosen.shape[0]
    block = rows * n_tp // nblk
    latent = lw.shape[1]
    bpd = rows // block
    bf16 = jnp.bfloat16
    hbm = pl.BlockSpec(memory_space=pltpu.HBM)
    vmem = pl.BlockSpec(memory_space=pltpu.VMEM)
    dma = pltpu.SemaphoreType.DMA
    piece = pltpu.VMEM((bpd, SPLIT, block, ow.shape[1] // SPLIT), bf16)
    arrays = [pltpu.with_memory_space_constraint(a, pltpu.HBM) for a in (tokens, qw, lw, ka, qg, lg, va, hg, ow, chosen)]
    return pl.pallas_call(
        functools.partial(kernel, n_kv),
        out_shape=jax.ShapeDtypeStruct((rows, ow.shape[1]), bf16),
        in_specs=[hbm] * 10,
        out_specs=vmem,
        scratch_shapes=[
            pltpu.VMEM((n_tp, rows, width), bf16),
            pltpu.VMEM(qw.shape, bf16),
            pltpu.VMEM(lw.shape, bf16),
            pltpu.VMEM(ka.shape, bf16),
            pltpu.VMEM(va.shape, bf16),
            pltpu.VMEM(ow.shape, bf16),
            pltpu.VMEM(qg.shape, bf16),
            pltpu.VMEM(lg.shape, bf16),
            pltpu.VMEM(hg.shape, bf16),
            pltpu.SMEM(chosen.shape, jnp.int32),
            pltpu.VMEM(chosen.shape, jnp.int32),
            pltpu.VMEM((nblk, block, latent), bf16),
            pltpu.VMEM((n_kv, 2, block // 2, latent), bf16),
            pltpu.VMEM((n_kv, block // 2, latent), bf16),
            pltpu.VMEM((n_kv,) + chosen.shape, jnp.int32),
            pltpu.VMEM((ka.shape[0], rows * n_tp, latent), bf16),
            piece,
            piece,
            piece,
            piece,
            piece,
            piece,
            dma((11,)),
            dma((3, bpd)),
            dma((3, bpd)),
            dma((1,)),
            dma((1,)),
            dma((3,)),
            dma((3,)),
            dma((n_kv,)),
            dma((n_kv,)),
            dma((n_kv,)),
            dma((n_kv,)),
            dma((n_kv,)),
            dma((n_kv,)),
            dma((3, bpd, SPLIT)),
            dma((3, bpd, SPLIT)),
        ],
        compiler_params=pltpu.CompilerParams(
            collective_id=0, has_side_effects=True, vmem_limit_bytes=50000000
        ),
    )(*arrays)


def solution(mesh):
    return jax.shard_map(
        functools.partial(body, mesh.shape["kv"], mesh.shape["tp"]),
        mesh=mesh,
        in_specs=(
            P(("kv", "tp"), None),
            P(None, "tp"),
            P(),
            P("tp", None, None),
            P(),
            P(),
            P("tp", None, None),
            P("tp", None),
            P("tp", None),
            P("kv", None),
        ),
        out_specs=P(("kv", "tp"), None),
        check_vma=False,
    )
```
